32 devices in a mesh: rep: 2 (over x), fs: 8 (over z, y), tp: 2 (over core).
Axes of the slice: x: 2, y: 2, z: 4, core: 2. Of those that a mesh axis runs over, the one named last changes fastest.
Arguments:
- inputs: bfloat16 [8192, 2048], P(('rep', 'fs')), may hold values from -6 to 6
- cotangent: bfloat16 [8192, 2048], P(('rep', 'fs')), may hold values from -6 to 6
- gate_pre: bfloat16 [8192, 5632], P(('rep', 'fs'), 'tp'), may hold values from -8 to 8
- up_pre: bfloat16 [8192, 5632], P(('rep', 'fs'), 'tp'), may hold values from -6 to 6
- gate_weight: float32 [2048, 5632], P('fs', 'tp'), may hold values from -0.125 to 0.125
- up_weight: float32 [2048, 5632], P('fs', 'tp'), may hold values from -0.125 to 0.125
- down_weight: float32 [2048, 5632], P('fs', 'tp'), may hold values from -0.078125 to 0.078125
- gate_scale: float32 [1, 5632], P(None, 'tp'), may hold values from 0.1 to 1.9
- up_scale: float32 [1, 5632], P(None, 'tp'), may hold values from 0.1 to 1.9
- down_scale: float32 [1, 5632], P(None, 'tp'), may hold values from 0.1 to 1.9
Outputs:
- input_grad: bfloat16 [8192, 2048], P(('rep', 'fs'), 'tp')
- gate_grad: float32 [2048, 5632], P('fs', 'tp')
- up_grad: float32 [2048, 5632], P('fs', 'tp')
- down_grad: float32 [2048, 5632], P('fs', 'tp')
The draws below stay inside these ranges and needn't reach their ends.
All inputs are finite; a program needn't handle non-finite values.
Results may differ from the reference program's by a relative error of at most 0.018.
Values may be sent and summed in bfloat16 or wider, within the bound.
A program may use at most 192 MiB of HBM per device.

```python
import jax
import jax.numpy as jnp
from jax import lax

D = 2048
FF = 5632
TOKENS = 8192
N_TP = 2


def spiked(array, own_key, source, target, blocks, factor):
    owner, partner = [(jnp.arange(array.shape[position]) // (array.shape[position] // blocks)).reshape([-1 if axis == position else 1 for axis in range(array.ndim)]) for position in (source, target)]
    chosen = jax.random.permutation(own_key, blocks)[partner]
    strong = (owner == chosen) | (owner == (partner + blocks // 2) % blocks)
    return jnp.where(strong, factor * array, array)


def level_of(key, extent, shards, least, top_value):
    factor_of, own = 1.0, jax.random.fold_in(key, 6)
    for axis_at, parts in shards:
        draws = jnp.exp(jax.random.uniform(jax.random.fold_in(own, axis_at), (parts,), jnp.float32, least / len(shards), top_value / len(shards)))
        factor_of = factor_of * jnp.repeat(draws, extent[axis_at] // parts).reshape([-1 if axis == axis_at else 1 for axis in range(len(extent))])
    return factor_of


def normal_values(own_key, extent, scale, reach, shards=(), kind=jnp.bfloat16):
    level = level_of(own_key, extent, shards, -0.22, 0.18) if shards else 1.0
    entries = jax.random.normal(own_key, extent, jnp.float32) * scale * level
    return jnp.minimum(jnp.maximum(entries, -reach), reach).astype(kind)


def heavy_noise(own_key, extent, deviation, reach, pieces, heavy, kind=jnp.bfloat16):
    result = deviation * jax.random.normal(own_key, extent, jnp.float32)
    if pieces:
        result = result * level_of(own_key, extent, pieces, -0.22, 0.18)
    return jnp.clip(spiked(result, jax.random.fold_in(own_key, 3), *heavy), -reach, reach).astype(kind)


def setup_inputs(seed: int = 0) -> dict:
    arg_keys = jax.random.split(jax.random.key(seed), 11)
    inputs = normal_values(arg_keys[0], (TOKENS, D), 1.0, 6.0, ((0, 16),))
    cotangent = heavy_noise(arg_keys[1], (TOKENS, D), 1.0, 6.0, ((0, 16),), (0, 1, 16, 2.0))
    gate_pre = normal_values(arg_keys[2], (TOKENS, FF), 1.5, 8.0, ((0, 16), (1, 2)))
    up_pre = normal_values(arg_keys[3], (TOKENS, FF), 1.0, 6.0, ((0, 16), (1, 2)))
    gate_weight = normal_values(arg_keys[4], (D, FF), D ** -0.5, 0.125, ((0, 8), (1, 2)), jnp.float32)
    up_weight = normal_values(arg_keys[5], (D, FF), D ** -0.5, 0.125, ((0, 8), (1, 2)), jnp.float32)
    down_weight = normal_values(arg_keys[6], (D, FF), FF ** -0.5, 0.078125, ((0, 8), (1, 2)), jnp.float32)
    gate_scale = jnp.clip(1.0 + 0.18 * jax.random.normal(arg_keys[7], (1, FF), jnp.float32), 0.1, 1.9)
    up_scale = jnp.clip(1.0 + 0.18 * jax.random.normal(arg_keys[8], (1, FF), jnp.float32), 0.1, 1.9)
    down_scale = jnp.clip(1.0 + 0.18 * jax.random.normal(arg_keys[9], (1, FF), jnp.float32), 0.1, 1.9)
    return dict(inputs=inputs, cotangent=cotangent, gate_pre=gate_pre, up_pre=up_pre, gate_weight=gate_weight, up_weight=up_weight, down_weight=down_weight, gate_scale=gate_scale, up_scale=up_scale, down_scale=down_scale)


def reference(inputs, cotangent, gate_pre, up_pre, gate_weight, up_weight, down_weight, gate_scale, up_scale, down_scale):
    gate = gate_pre.astype(jnp.float32)
    upper = up_pre.astype(jnp.float32)
    sig = jax.nn.sigmoid(gate)
    act = gate * sig
    hidden = (act * upper).astype(jnp.bfloat16)
    down_bf = down_weight.astype(jnp.bfloat16)
    hidden_cot = jnp.dot(cotangent, down_bf, preferred_element_type=jnp.float32) * down_scale
    gate_cot = (hidden_cot * upper * sig * (1.0 + gate * (1.0 - sig)) * gate_scale).astype(jnp.bfloat16)
    up_cot = (hidden_cot * act * up_scale).astype(jnp.bfloat16)
    width = FF // N_TP
    gate_bf = gate_weight.astype(jnp.bfloat16)
    up_bf = up_weight.astype(jnp.bfloat16)

    def block_sum(total, index):
        start = (index * width).astype(jnp.int32)
        gc = lax.dynamic_slice_in_dim(gate_cot, start, width, 1)
        uc = lax.dynamic_slice_in_dim(up_cot, start, width, 1)
        gw = lax.dynamic_slice_in_dim(gate_bf, start, width, 1)
        uw = lax.dynamic_slice_in_dim(up_bf, start, width, 1)
        part = jnp.dot(gc, gw.T, preferred_element_type=jnp.float32) + jnp.dot(uc, uw.T, preferred_element_type=jnp.float32)
        return total + part.astype(jnp.bfloat16).astype(jnp.float32), None

    summed, _ = lax.scan(block_sum, jnp.zeros((TOKENS, D), jnp.float32), jnp.arange(N_TP, dtype=jnp.int32))
    input_grad = summed.astype(jnp.bfloat16)
    gate_grad = jnp.dot(inputs.T, gate_cot, preferred_element_type=jnp.float32)
    up_grad = jnp.dot(inputs.T, up_cot, preferred_element_type=jnp.float32)
    down_grad = jnp.dot(cotangent.T, hidden, preferred_element_type=jnp.float32) * down_scale
    return (input_grad, gate_grad, up_grad, down_grad)
```

```python
import functools

import jax
import jax.numpy as jnp
from jax import lax
from jax.sharding import PartitionSpec as P


BF = jnp.bfloat16
F32 = jnp.float32


def local(
    n_rep,
    n_fs,
    n_tp,
    inputs,
    cotangent,
    gate_pre,
    up_pre,
    gate_weight,
    up_weight,
    down_weight,
    gate_scale,
    up_scale,
    down_scale,
):
    n_out = 4 if n_fs % 4 == 0 else 1
    n_in = n_fs // n_out
    tokens = inputs.shape[0]
    width = inputs.shape[1]
    block = width // n_fs
    part = gate_pre.shape[1] // n_rep
    r = lax.axis_index("rep")
    f = lax.axis_index("fs")
    t = lax.axis_index("tp")
    zo, yo = f // n_in, f % n_in

    def from_rep(value, k):
        return lax.ppermute(value, "rep", [((i + k) % n_rep, i) for i in range(n_rep)])

    def from_tp(value, k):
        return lax.ppermute(value, "tp", [((i + k) % n_tp, i) for i in range(n_tp)])

    def from_outer(value, k):
        pairs = [
            (((z + k) % n_out) * n_in + y, z * n_in + y)
            for z in range(n_out)
            for y in range(n_in)
        ]
        return lax.ppermute(value, "fs", pairs)

    def from_inner(value, k):
        pairs = [
            (z * n_in + (y + k) % n_in, z * n_in + y)
            for z in range(n_out)
            for y in range(n_in)
        ]
        return lax.ppermute(value, "fs", pairs)

    def column_part(value, index):
        return lax.dynamic_slice_in_dim(value, index * part, part, 1)

    def spread_tokens(value):
        return jnp.concatenate([value] + [from_rep(value, k) for k in range(1, n_rep)], axis=0)

    def exchange_parts(value):
        pieces = [column_part(value, r)]
        for k in range(1, n_rep):
            pieces.append(from_rep(column_part(value, (r - k + n_rep) % n_rep), k))
        return jnp.concatenate(pieces, axis=0)

    def rotate(value):
        result = []
        for j in range(n_in):
            cuts = [
                lax.dynamic_slice_in_dim(
                    value, (((zo + i) % n_out) * n_in + (yo + j) % n_in) * block, block, 1
                )
                for i in range(n_out)
            ]
            result.append(jnp.concatenate(cuts, axis=1))
        return jnp.concatenate(result, axis=1)

    def gather_rows(own):
        line = [own] + [from_outer(own, i) for i in range(1, n_out)]
        blocks = list(line)
        for j in range(1, n_in):
            blocks += [from_inner(b, j) for b in line]
        return jnp.concatenate(blocks, axis=0)

    down_all = gather_rows(column_part(down_weight, r).astype(BF))
    gate = exchange_parts(gate_pre).astype(F32)
    upper = exchange_parts(up_pre).astype(F32)
    ys = spread_tokens(rotate(cotangent))
    xs = spread_tokens(rotate(inputs))
    gs, us, ds = (column_part(s, r) for s in (gate_scale, up_scale, down_scale))

    sig = jax.nn.sigmoid(gate)
    act = gate * sig
    hidden = (act * upper).astype(BF)
    hidden_cot = jnp.dot(ys, down_all, preferred_element_type=F32) * ds
    gate_cot = (hidden_cot * upper * sig * (1.0 + gate * (1.0 - sig)) * gs).astype(BF)
    up_cot = (hidden_cot * act * us).astype(BF)
    both_cot = jnp.concatenate([gate_cot, up_cot], axis=1)

    dims = (((0,), (0,)), ((), ()))
    stretch = n_out * block

    def scattered(left, right, scale):
        def piece(j):
            value = lax.dot_general(
                left[:, j * stretch : (j + 1) * stretch], right, dims, preferred_element_type=F32
            )
            if scale is not None:
                value = value * scale
            return value

        arrived = []
        for j in range(1, n_in):
            arrived.append(from_inner(piece(j).astype(BF), n_in - j))
        total = piece(0)
        for value in arrived:
            total = total + value.astype(F32)
        own = total[:block]
        sent = total[block:].astype(BF)
        for i in range(1, n_out):
            own = own + from_outer(sent[(i - 1) * block : i * block], n_out - i).astype(F32)
        return lax.reduce_precision(own, 8, 7)

    def whole_columns(own):
        result = jnp.zeros((block, part * n_rep), F32)
        narrow = own.astype(BF)
        result = lax.dynamic_update_slice_in_dim(result, own, r * part, 1)
        for k in range(1, n_rep):
            value = from_rep(narrow, k).astype(F32)
            result = lax.dynamic_update_slice_in_dim(result, value, ((r + k) % n_rep) * part, 1)
        return result

    down_grad = whole_columns(scattered(ys, hidden, ds))
    gate_grad = whole_columns(scattered(xs, gate_cot, None))
    up_grad = whole_columns(scattered(xs, up_cot, None))

    both_rows = jnp.concatenate([column_part(gate_weight, r), column_part(up_weight, r)], axis=1)
    both_all = gather_rows(both_rows.astype(BF))
    partial = lax.dot_general(
        both_cot, both_all, (((1,), (1,)), ((), ())), preferred_element_type=F32
    ).astype(BF)
    back = []
    for z in range(n_out):
        for y in range(n_in):
            i = (z - zo + n_out) % n_out
            j = (y - yo + n_in) % n_in
            back.append(lax.dynamic_slice_in_dim(partial, (j * n_out + i) * block, block, 1))
    partial = jnp.concatenate(back, axis=1)
    share = width // n_tp
    total = lax.dynamic_slice_in_dim(partial, t * share, share, 1).astype(F32)
    for k in range(1, n_tp):
        target = (t - k + n_tp) % n_tp
        total = total + from_tp(
            lax.dynamic_slice_in_dim(partial, target * share, share, 1), k
        ).astype(F32)
    grad = total[:tokens]
    away = total[tokens:].astype(BF)
    for k in range(1, n_rep):
        grad = grad + from_rep(away[(k - 1) * tokens : k * tokens], n_rep - k).astype(F32)
    return (grad.astype(BF), gate_grad, up_grad, down_grad)


def solution(mesh):
    sizes = mesh.shape
    return jax.shard_map(
        functools.partial(local, sizes["rep"], sizes["fs"], sizes["tp"]),
        mesh=mesh,
        in_specs=(
            P(("rep", "fs"), None),
            P(("rep", "fs"), None),
            P(("rep", "fs"), "tp"),
            P(("rep", "fs"), "tp"),
            P("fs", "tp"),
            P("fs", "tp"),
            P("fs", "tp"),
            P(None, "tp"),
            P(None, "tp"),
            P(None, "tp"),
        ),
        out_specs=(P(("rep", "fs"), "tp"), P("fs", "tp"), P("fs", "tp"), P("fs", "tp")),
        check_vma=False,
    )
```
